32 devices in a mesh: grp: 1, ep: 16 (over z, y, x), tp: 2 (over core).
Axes of the slice: x: 2, y: 2, z: 4, core: 2. Of those that a mesh axis runs over, the one named last changes fastest.
Arguments:
- tokens_in: bfloat16 [1024, 2048], P(('grp', 'ep')), may hold values from -6 to 6
- norm_gain: float32 [2048], replicated, may hold values from 0.1 to 1.9
- gate_proj: bfloat16 [16, 2048, 1024], P('ep', None, 'tp'), may hold values from -0.125 to 0.125
- up_proj: bfloat16 [16, 2048, 1024], P('ep', None, 'tp'), may hold values from -0.125 to 0.125
- down_proj: bfloat16 [16, 1024, 2048], P('ep', 'tp'), may hold values from -0.1875 to 0.1875
- route_ids: int32 [1024, 8], P(('grp', 'ep')), may hold values from 0 to 15, all different within a row; in each aligned block of 64 rows (0 to 63, 64 to 127, ...) at most 64 rows name the same one
- group_weight: float32 [1024, 2], P(('grp', 'ep')), may hold values from 0.05 to 1
- expert_weight: float32 [1024, 8], P(('grp', 'ep')), may hold values from 0.05 to 1
Outputs:
- expert_mix: bfloat16 [1024, 2048], P(('grp', 'ep'), 'tp')
The draws below stay inside these ranges and needn't reach their ends.
Inputs may be any that keep to these rules, and one draw needn't show every extreme that they name: `route_ids`: each row names 8 different experts; within the rows of one index of ep no expert is named by more than 64 rows, a bound that some of them reach.
All inputs are finite; a program needn't handle non-finite values.
Results may differ from the reference program's by a relative error of at most 0.0077.
Values may be sent and summed in bfloat16 or wider, within the bound.
A program may use at most 64 MiB of HBM per device.

```python
import math
import jax
import jax.numpy as jnp
import numpy as np
from jax import lax

D = 2048
DE = 1024
TOP = 8
EXP_GRP = 8
TOK_DEV = 64
EXPERTS = 16
GROUPS = 2
CAP = 64
TOKENS = 1024
N_EP = 16
N_TP = 2


def steps_of(own_key, dims, shards, smallest, largest):
    loudness = 1.0
    for axis_at, shards_of in shards:
        draws = jax.random.uniform(jax.random.fold_in(jax.random.fold_in(own_key, 6), axis_at), (shards_of,), jnp.float32, smallest / len(shards), largest / len(shards))
        loudness = loudness * jnp.repeat(jnp.exp(draws), dims[axis_at] // shards_of).reshape((-1,) + (1,) * (len(dims) - 1 - axis_at))
    return loudness


def shared_out(key, own, number, rows, count, top, most, skew):
    ranking = jax.random.permutation(key, count)
    crowded, usual = load_shares(count, rows * top, most, skew, True), load_shares(count, rows * top, most, skew, False)
    places = jnp.arange(count)

    def named(sizes, offset_by):
        used = int((sizes > 0).sum())
        fixed = max(1, used // 4)
        passed = fixed + (places - fixed + offset_by * (used - fixed)) % max(1, count - fixed)
        return jnp.zeros((count,), jnp.int32).at[ranking[jnp.where(places < fixed, places, passed)]].set(jnp.asarray(sizes, jnp.int32))

    sizes = jnp.where(number % 4 == 0, named(crowded, number // 4), named(usual, number - number // 4 - 1))
    mixed = jax.random.permutation(jax.random.fold_in(own, 3), count)
    giver, receiver = mixed[0:count // 2 * 2:2], mixed[1:count // 2 * 2:2]
    margin = jnp.minimum(sizes[giver] - 1, most - sizes[receiver]) // 2
    margin = jnp.where((giver == ranking[0]) | (receiver == ranking[0]) | (sizes[receiver] == 0), 0, jnp.maximum(margin, 0))
    passed = jax.random.randint(jax.random.fold_in(own, 4), (count // 2,), 0, 1 << 20) % (margin + 1)
    sizes = sizes.at[giver].add(-passed).at[receiver].add(passed)
    labels = jnp.searchsorted(jnp.cumsum(sizes), jnp.arange(rows * top), side="right").astype(jnp.int32)
    grid = labels.reshape(top, rows).T
    grid = grid[jax.random.permutation(jax.random.fold_in(own, 1), rows)]
    offset_by = jax.random.randint(jax.random.fold_in(own, 2), (rows, 1), 0, top)
    return jnp.take_along_axis(grid, (jnp.arange(top)[None, :] + offset_by) % top, axis=1)


def load_shares(number_of, total, limit, skew, full):
    portions = [(1 << 20) // math.isqrt(standing ** skew) + 1 for standing in range(1, number_of + 1)]
    largest = limit if full else min(limit, max(-(-total // number_of), total * portions[0] // sum(portions)))
    least = 1 if total - largest >= number_of - 1 else 0
    given, spare = [largest] + [least] * (number_of - 1), total - largest - least * (number_of - 1)
    while spare > 0:
        free = [i for i in range(1, number_of) if given[i] < largest] or [i for i in range(1, number_of) if given[i] < limit]
        mass, left = sum([portions[i] for i in free]), spare
        for i in free:
            addition = min(limit - given[i], max(1, left * portions[i] // mass), spare)
            given[i] = given[i] + addition
            spare = spare - addition
    return np.array(given)


def noise(stream_key, dims, deviation, limit, split=(), kind=jnp.bfloat16):
    drawn = jax.random.normal(stream_key, dims, jnp.float32) * deviation
    if len(split) > 0:
        drawn = steps_of(stream_key, dims, split, -0.22, 0.18) * drawn
    return jnp.clip(drawn, min=-limit, max=limit).astype(kind)


def setup_inputs(seed: int = 0, part: int = 0) -> dict:
    arg_keys = jax.random.split(jax.random.key(seed), 9)
    own_keys = jax.random.split(jax.random.fold_in(arg_keys[8], part), 9)
    tokens_in = noise(own_keys[0], (TOKENS, D), 1.0, 6.0, ((0, 16),))
    norm_gain = jnp.clip(1.0 + 0.18 * jax.random.normal(arg_keys[1], (D,), jnp.float32), 0.1, 1.9)
    gate_proj = noise(arg_keys[2], (EXPERTS, D, DE), D ** -0.5, 0.125, ((0, 16), (2, 2)))
    up_proj = noise(arg_keys[3], (EXPERTS, D, DE), D ** -0.5, 0.125, ((0, 16), (2, 2)))
    down_proj = noise(arg_keys[4], (EXPERTS, DE, D), DE ** -0.5, 0.1875, ((0, 16), (1, 2)))
    route_ids_keys = jax.random.split(jax.random.fold_in(own_keys[5], 1), TOKENS // TOK_DEV)
    route_ids_turns = jax.random.permutation(jax.random.fold_in(own_keys[5], 3), TOKENS // TOK_DEV)
    route_ids = jax.vmap(lambda own, number: shared_out(jax.random.fold_in(own_keys[5], 2), own, number, TOK_DEV, EXPERTS, TOP, CAP, 2))(route_ids_keys, route_ids_turns).reshape((TOKENS, TOP))
    group_weight = jnp.clip(jnp.exp(math.log(1.0) - 2.9957323 * jax.random.uniform(own_keys[6], (TOKENS, GROUPS), jnp.float32) ** steps_of(own_keys[6], (TOKENS, GROUPS), ((0, 16),), -0.2, 0.2)), 0.05, 1.0)
    expert_weight = jnp.clip(jnp.exp(math.log(1.0) - 2.9957323 * jax.random.uniform(own_keys[7], (TOKENS, TOP), jnp.float32) ** steps_of(own_keys[7], (TOKENS, TOP), ((0, 16),), -0.2, 0.2)), 0.05, 1.0)
    return dict(tokens_in=tokens_in, norm_gain=norm_gain, gate_proj=gate_proj, up_proj=up_proj, down_proj=down_proj, route_ids=route_ids, group_weight=group_weight, expert_weight=expert_weight)


EPSILON = 1e-06

def reference(tokens_in, norm_gain, gate_proj, up_proj, down_proj, route_ids, group_weight, expert_weight):
    row_values = tokens_in.astype(jnp.float32)
    inv_scale = lax.rsqrt(lax.optimization_barrier(jnp.mean(row_values * row_values, axis=-1, keepdims=True)) + EPSILON)
    normed = (row_values * inv_scale * norm_gain.astype(jnp.float32)).astype(jnp.bfloat16)
    token_count = tokens_in.shape[0]
    expert_count = gate_proj.shape[0]
    route_count = token_count * TOP
    flat_ids = route_ids.reshape(route_count).astype(jnp.int32)
    sort_order = jnp.argsort(flat_ids, stable=True).astype(jnp.int32)
    expert_counts = lax.optimization_barrier(jnp.sum((flat_ids[None, :] == jnp.arange(expert_count, dtype=jnp.int32)[:, None]).astype(jnp.int32), axis=1)).astype(jnp.int32)
    expert_starts = (jnp.cumsum(expert_counts) - expert_counts).astype(jnp.int32)
    buffer_rows = N_EP * CAP
    padded_order = jnp.concatenate([sort_order, jnp.zeros((buffer_rows,), jnp.int32)])
    half_width = DE // N_TP

    def one_expert(expert_index):
        begin_at = expert_starts[expert_index].astype(jnp.int32)
        picked = lax.dynamic_slice_in_dim(padded_order, begin_at, buffer_rows)
        is_valid = jnp.arange(buffer_rows, dtype=jnp.int32) < expert_counts[expert_index]
        source_rows = normed[picked // TOP]
        gate_acts = jnp.dot(source_rows, gate_proj[expert_index], preferred_element_type=jnp.float32)
        up_acts = jnp.dot(source_rows, up_proj[expert_index], preferred_element_type=jnp.float32)
        hidden = (jax.nn.silu(gate_acts) * up_acts).astype(jnp.bfloat16)
        total_sum = jnp.zeros((buffer_rows, D), jnp.float32)
        for lane_block in range(N_TP):
            part_sum = jnp.dot(hidden[:, lane_block * half_width:(lane_block + 1) * half_width], down_proj[expert_index, lane_block * half_width:(lane_block + 1) * half_width], preferred_element_type=jnp.float32)
            part_sum = lax.optimization_barrier(part_sum.astype(jnp.bfloat16))
            total_sum = total_sum + part_sum.astype(jnp.float32)
        target_rows = jnp.where(is_valid, picked, route_count).astype(jnp.int32)
        return (total_sum.astype(jnp.bfloat16), target_rows)
    outputs, targets = lax.map(one_expert, jnp.arange(expert_count, dtype=jnp.int32))
    per_route = jnp.zeros((route_count + 1, D), jnp.bfloat16).at[targets.reshape(-1)].set(outputs.reshape(-1, D))[:route_count]
    chosen = per_route.reshape(token_count, TOP, D).astype(jnp.float32)
    group_ids = (route_ids // EXP_GRP).astype(jnp.int32)
    group_part = jnp.take_along_axis(group_weight, group_ids, axis=1)
    gate_values = group_part * expert_weight / lax.optimization_barrier(jnp.sum(expert_weight, axis=1, keepdims=True))
    return lax.optimization_barrier(jnp.sum(chosen * gate_values[:, :, None], axis=1)).astype(jnp.bfloat16)
```

```python
import jax
import jax.numpy as jnp
from jax import lax
from jax.sharding import PartitionSpec as P

EXP_GRP = 8


EPSILON = 1e-06


def on_device(
    tokens_in, norm_gain, gate_proj, up_proj, down_proj, route_ids, group_weight, expert_weight
):
    token_count, model_width = tokens_in.shape
    expert_count = gate_proj.shape[0] * lax.axis_size("ep")
    lane_count = lax.axis_size("tp")
    lane_index = lax.axis_index("tp")
    share = token_count // lane_count
    own_rows = lax.dynamic_slice_in_dim(tokens_in, lane_index * share, share, 0)
    row_values = own_rows.astype(jnp.float32)
    inv_scale = lax.rsqrt(jnp.mean(row_values * row_values, axis=-1, keepdims=True) + EPSILON)
    normed = (row_values * inv_scale * norm_gain).astype(jnp.bfloat16)
    rows = lax.all_gather(normed, ("ep", "tp"), axis=0, tiled=True)
    experts = jnp.arange(expert_count, dtype=jnp.int32)
    share_of = expert_weight / jnp.sum(expert_weight, axis=1, keepdims=True)
    named = route_ids[:, :, None] == experts[None, None, :]
    chosen = jnp.sum(jnp.where(named, share_of[:, :, None], 0.0), axis=1)
    gates = chosen * jnp.repeat(group_weight, EXP_GRP, axis=1)
    all_gates = lax.all_gather(gates, "ep", axis=0, tiled=True)
    own_gate = lax.dynamic_slice_in_dim(all_gates, lax.axis_index("ep"), 1, 1)
    gate_acts = jnp.dot(rows, gate_proj[0], preferred_element_type=jnp.float32)
    up_acts = jnp.dot(rows, up_proj[0], preferred_element_type=jnp.float32)
    hidden = (jax.nn.silu(gate_acts) * up_acts).astype(jnp.bfloat16)
    partial_rows = jnp.dot(hidden, down_proj[0], preferred_element_type=jnp.float32)
    weighted = (partial_rows * own_gate).astype(jnp.bfloat16)
    halves = lax.psum_scatter(weighted, "tp", scatter_dimension=1, tiled=True)
    return lax.psum_scatter(halves, "ep", scatter_dimension=0, tiled=True)


def solution(mesh):
    in_specs = (
        P(("grp", "ep"), None),
        P(),
        P("ep", None, "tp"),
        P("ep", None, "tp"),
        P("ep", "tp", None),
        P(("grp", "ep"), None),
        P(("grp", "ep"), None),
        P(("grp", "ep"), None),
    )
    out_specs = P(("grp", "ep"), "tp")
    return jax.shard_map(
        on_device, mesh=mesh, in_specs=in_specs, out_specs=out_specs, check_vma=False
    )
```

```python
import functools

import jax
import jax.numpy as jnp
from jax import lax
from jax.experimental import pallas as pl
from jax.experimental.pallas import tpu as pltpu
from jax.sharding import PartitionSpec as P

TOP = 8
EXP_GRP = 8


EPSILON = 1e-06

MESH = pl.DeviceIdType.MESH
PLANE = 4
DEPTH = 4


def on_device(
    tokens_in, norm_gain, gate_proj, up_proj, down_proj, route_ids, group_weight, expert_weight
):
    token_count, model_width = tokens_in.shape
    expert_count = gate_proj.shape[0] * lax.axis_size("ep")
    lane_count = lax.axis_size("tp")
    part_width = model_width // lane_count
    capacity = min(token_count, max(2, 2 * token_count * TOP // expert_count))
    slot_total = expert_count * capacity
    row_values = tokens_in.astype(jnp.float32)
    inv_scale = lax.rsqrt(jnp.mean(row_values * row_values, axis=-1, keepdims=True) + EPSILON)
    normed = (row_values * inv_scale * norm_gain).astype(jnp.bfloat16)
    route_count = token_count * TOP
    flat_ids = route_ids.reshape(route_count)
    positions = jnp.arange(route_count, dtype=jnp.int32)
    same_expert = (flat_ids[:, None] == flat_ids[None, :]) & (
        positions[None, :] < positions[:, None]
    )
    slot_rank = jnp.sum(same_expert.astype(jnp.int32), axis=1)
    slot_index = flat_ids * capacity + slot_rank
    slot_match = jnp.arange(slot_total, dtype=jnp.int32)[:, None] == slot_index[None, :]
    selector = jnp.sum(
        slot_match.reshape(slot_total, token_count, TOP).astype(jnp.int32), axis=2
    ).astype(jnp.bfloat16)
    gate_local = gate_proj[0]
    up_local = up_proj[0]
    lane_index = lax.axis_index("tp")
    own_half = lax.dynamic_slice_in_dim(normed, lane_index * part_width, part_width, 1)
    outgoing = jnp.dot(selector, own_half, preferred_element_type=jnp.float32).astype(jnp.bfloat16)
    arrived = lax.all_to_all(
        outgoing.reshape(expert_count, capacity, part_width),
        "ep",
        split_axis=0,
        concat_axis=0,
        tiled=True,
    )
    arrived = arrived.reshape(slot_total, part_width)
    column_piece = lax.all_gather(arrived, "tp", axis=1, tiled=True)
    gate_acts = jnp.dot(column_piece, gate_local, preferred_element_type=jnp.float32)
    up_acts = jnp.dot(column_piece, up_local, preferred_element_type=jnp.float32)
    hidden = (jax.nn.silu(gate_acts) * up_acts).astype(jnp.bfloat16)
    partial_rows = jnp.dot(hidden, down_proj[0], preferred_element_type=jnp.float32)
    summed = lax.psum_scatter(
        partial_rows.reshape(expert_count, capacity, model_width).astype(jnp.bfloat16),
        "tp",
        scatter_dimension=2,
        tiled=True,
    )
    returned = lax.all_to_all(summed, "ep", split_axis=0, concat_axis=0, tiled=True).reshape(
        slot_total, part_width
    )
    picked = returned[slot_index].astype(jnp.float32).reshape(token_count, TOP, part_width)
    group_ids = route_ids // EXP_GRP
    group_count = group_weight.shape[1]
    group_match = (
        group_ids[:, :, None] == jnp.arange(group_count, dtype=jnp.int32)[None, None, :]
    ).astype(jnp.float32)
    group_part = jnp.sum(group_weight[:, None, :] * group_match, axis=2)
    gate_values = group_part * expert_weight / jnp.sum(expert_weight, axis=1, keepdims=True)
    return jnp.sum(picked * gate_values[:, :, None], axis=1).astype(jnp.bfloat16)


def plane_order(step, z):
    if step == 0:
        return z
    if step == 1:
        return z + 1 - 2 * (z % 2)
    far = DEPTH - 1 - (DEPTH - 1) * (z // 2)
    return far + (1 - 2 * (1 - z // 2)) * (DEPTH - 1 - step)


def kernel(
    expert_total, tokens_ref, gain_ref, gate_hbm, up_hbm, down_hbm, ids_ref, group_ref, weight_ref,
    out_ref,
    rows, gate_w, up_w, down_w, own_part, give, got, diag_out, diag_x, diag_y, x_out, y_out,
    x_in, y_in, z_total, z_out, z_below, z_above,
    w_sem, up_s, dn_s, z_r, gx_s, gx_r, gy_s, gy_r, dx_s, dx_r, dy_s, dy_r, sib_s, sib_r,
    tp_s, tp_r, rdx_s, rdx_r, rdy_s, rdy_r, rx_s, rx_r, ry_s, ry_r, rz_s, rzb_r, rza_r,
):
    me = lax.axis_index("ep")
    core = lax.axis_index("tp")
    z, q = me // PLANE, me % PLANE
    y, x = q // 2, q % 2
    qx, qy, qd = y * 2 + 1 - x, (1 - y) * 2 + x, (1 - y) * 2 + 1 - x
    x_peer, y_peer = {"ep": z * PLANE + qx}, {"ep": z * PLANE + qy}
    up_peer, dn_peer = {"ep": me + PLANE}, {"ep": me - PLANE}
    sibling = {"tp": 1 - core}
    has_up, has_dn = z < DEPTH - 1, z > 0
    half_rows, width = tokens_ref.shape[0] // 2, tokens_ref.shape[1]
    sub = half_rows // 2
    block = 2 * half_rows
    part = width // 2
    always = None
    sent = []

    weight_copies = [
        pltpu.make_async_copy(src.at[0], dst, w_sem.at[i])
        for i, (src, dst) in enumerate(((gate_hbm, gate_w), (up_hbm, up_w), (down_hbm, down_w)))
    ]
    for copy in weight_copies:
        copy.start()

    barrier = pltpu.get_barrier_semaphore()
    for peer in (x_peer, y_peer, sibling):
        pl.semaphore_signal(barrier, inc=1, device_id=peer, device_id_type=MESH)

    @pl.when(has_up)
    def _():
        pl.semaphore_signal(barrier, inc=1, device_id=up_peer, device_id_type=MESH)

    @pl.when(has_dn)
    def _():
        pl.semaphore_signal(barrier, inc=1, device_id=dn_peer, device_id_type=MESH)

    def send(src, dst, send_sem, recv_sem, peer, when=always):
        copy = pltpu.make_async_remote_copy(
            src_ref=src, dst_ref=dst, send_sem=send_sem, recv_sem=recv_sem,
            device_id=peer, device_id_type=MESH,
        )
        sent.append((copy, when))
        if when is None:
            copy.start()
        else:
            pl.when(when)(copy.start)

    def arrive(dst, recv_sem):
        pltpu.make_async_remote_copy(
            src_ref=dst, dst_ref=dst, send_sem=recv_sem, recv_sem=recv_sem,
            device_id=sibling, device_id_type=MESH,
        ).wait_recv()

    begin = pl.multiple_of(core * half_rows, half_rows)
    values = tokens_ref[pl.ds(begin, half_rows), :].astype(jnp.float32)
    scale = lax.rsqrt(jnp.mean(values * values, axis=-1, keepdims=True) + EPSILON)
    normed = (values * scale * gain_ref[...]).astype(jnp.bfloat16)
    lane = lax.broadcasted_iota(jnp.int32, (half_rows, 128), 1)
    expert = lane % expert_total
    ids = ids_ref[pl.ds(begin, half_rows), :]
    weights = weight_ref[pl.ds(begin, half_rows), :]
    groups = group_ref[pl.ds(begin, half_rows), :]
    weights = weights / jnp.sum(weights, axis=1, keepdims=True)
    gates = jnp.zeros((half_rows, 128), jnp.float32)
    for k in range(TOP):
        gates = gates + jnp.where(ids[:, k : k + 1] == expert, weights[:, k : k + 1], 0.0)
    group_part = jnp.zeros((half_rows, 128), jnp.float32)
    for g in range(groups.shape[1]):
        group_part = jnp.where(expert // EXP_GRP == g, groups[:, g : g + 1], group_part)
    gates = gates * group_part
    high = gates.astype(jnp.bfloat16).astype(jnp.float32)
    middle = (gates - high).astype(jnp.bfloat16).astype(jnp.float32)
    low = gates - high - middle
    third = lane // expert_total
    tail = jnp.where(
        third == 0, high, jnp.where(third == 1, middle, jnp.where(third == 2, low, 0.0))
    ).astype(jnp.bfloat16)
    for p in range(2):
        rows[z, q, core, p, :, 0:width] = normed[p * sub : (p + 1) * sub]
        rows[z, q, core, p, :, width:] = tail[p * sub : (p + 1) * sub]

    pl.semaphore_wait(barrier, 3 + jnp.minimum(z, 1) + jnp.minimum(DEPTH - 1 - z, 1))

    def own_column(step):
        at = plane_order(step, z)
        for p in range(2):
            piece = rows.at[at, q, core, p]
            if step > 0:
                arrive(piece, z_r.at[at, p])
            send(piece, piece, up_s.at[at, p], z_r.at[at, p], up_peer, has_up & (at <= z))
            send(piece, piece, dn_s.at[at, p], z_r.at[at, p], dn_peer, has_dn & (at >= z))
            send(piece, piece, gx_s.at[at, p], gx_r.at[at, p], x_peer)
            send(piece, piece, gy_s.at[at, p], gy_r.at[at, p], y_peer)
        to_sibling(at, q)

    def to_sibling(at, column):
        piece = rows.at[at, column, core]
        send(piece, piece, sib_s.at[at, column], sib_r.at[at, column], sibling)

    def neighbours(step):
        at = plane_order(step, z)
        arrive(rows.at[at, qx, core, 0], gx_r.at[at, 0])
        piece = rows.at[at, qx, core, 0]
        send(piece, piece, dy_s.at[at], dy_r.at[at], y_peer)
        arrive(rows.at[at, qy, core, 1], gy_r.at[at, 1])
        piece = rows.at[at, qy, core, 1]
        send(piece, piece, dx_s.at[at], dx_r.at[at], x_peer)
        arrive(rows.at[at, qx, core, 1], gx_r.at[at, 1])
        to_sibling(at, qx)
        arrive(rows.at[at, qy, core, 0], gy_r.at[at, 0])
        to_sibling(at, qy)

    def diagonal(step):
        at = plane_order(step, z)
        arrive(rows.at[at, qd, core, 0], dy_r.at[at])
        arrive(rows.at[at, qd, core, 1], dx_r.at[at])
        to_sibling(at, qd)

    mine = pl.multiple_of(core * part, part)
    other = pl.multiple_of((1 - core) * part, part)

    def compute(step):
        at = plane_order(step, z)
        for column in range(PLANE):
            arrive(rows.at[at, column, 1 - core], sib_r.at[at, column])
        if step == 0:
            for copy in weight_copies:
                copy.wait()
        count = PLANE * block
        taken = rows[at, :, :, :, :, 0:width].reshape(count, width)
        gate_acts = jnp.dot(taken, gate_w[...], preferred_element_type=jnp.float32)
        up_acts = jnp.dot(taken, up_w[...], preferred_element_type=jnp.float32)
        hidden = (gate_acts / (1.0 + jnp.exp(-gate_acts)) * up_acts).astype(jnp.bfloat16)
        tails = rows[at, :, :, :, :, width:].reshape(count, 128).astype(jnp.float32)
        lanes = lax.broadcasted_iota(jnp.int32, (count, 128), 1)
        wanted = (lanes % expert_total == me) & (lanes < 3 * expert_total)
        gate = jnp.sum(jnp.where(wanted, tails, 0.0), axis=1, keepdims=True)
        theirs = jnp.dot(hidden, down_w[:, pl.ds(other, part)], preferred_element_type=jnp.float32)
        give[at] = (theirs * gate).astype(jnp.bfloat16).reshape(PLANE, block, part)
        send(give.at[at], got.at[at], tp_s.at[at], tp_r.at[at], sibling)
        ours = jnp.dot(hidden, down_w[:, pl.ds(mine, part)], preferred_element_type=jnp.float32)
        own_part[at] = (ours * gate).reshape(PLANE, block, part)

    def pair_sum(at, column):
        return own_part[at, column] + got[at, column].astype(jnp.float32)

    def give_diagonal(step):
        at = plane_order(step, z)
        arrive(got.at[at], tp_r.at[at])
        diag_out[at] = pair_sum(at, qd).astype(jnp.bfloat16).reshape(2, half_rows, part)
        send(diag_out.at[at, 0], diag_x.at[at], rdx_s.at[at], rdx_r.at[at], x_peer)
        send(diag_out.at[at, 1], diag_y.at[at], rdy_s.at[at], rdy_r.at[at], y_peer)

    def give_neighbours(step):
        at = plane_order(step, z)
        arrive(diag_x.at[at], rdx_r.at[at])
        total = pair_sum(at, qy)
        y_out[at, 0:half_rows] = (
            total[0:half_rows] + diag_x[at].astype(jnp.float32)
        ).astype(jnp.bfloat16)
        y_out[at, half_rows:] = total[half_rows:].astype(jnp.bfloat16)
        send(y_out.at[at], y_in.at[at], ry_s.at[at], ry_r.at[at], y_peer)
        arrive(diag_y.at[at], rdy_r.at[at])
        total = pair_sum(at, qx)
        x_out[at, 0:half_rows] = total[0:half_rows].astype(jnp.bfloat16)
        x_out[at, half_rows:] = (
            total[half_rows:] + diag_y[at].astype(jnp.float32)
        ).astype(jnp.bfloat16)
        send(x_out.at[at], x_in.at[at], rx_s.at[at], rx_r.at[at], x_peer)

    def give_column(step):
        at = plane_order(step, z)
        arrive(x_in.at[at], rx_r.at[at])
        arrive(y_in.at[at], ry_r.at[at])
        z_total[...] = (
            pair_sum(at, q) + x_in[at].astype(jnp.float32) + y_in[at].astype(jnp.float32)
        )

        @pl.when(has_dn & (at >= z))
        def _():
            arrive(z_below.at[at], rzb_r.at[at])
            z_total[...] += z_below[at].astype(jnp.float32)

        @pl.when(has_up & (at <= z))
        def _():
            arrive(z_above.at[at], rza_r.at[at])
            z_total[...] += z_above[at].astype(jnp.float32)

        if step == 0:
            out_ref[...] = z_total[...].astype(jnp.bfloat16)
        else:
            z_out[at] = z_total[...].astype(jnp.bfloat16)
            send(z_out.at[at], z_below.at[at], rz_s.at[at], rzb_r.at[at], up_peer, at > z)
            send(z_out.at[at], z_above.at[at], rz_s.at[at], rza_r.at[at], dn_peer, at < z)

    own_column(0)
    own_column(1)
    neighbours(0)
    own_column(2)
    neighbours(1)
    diagonal(0)
    own_column(3)
    neighbours(2)
    diagonal(1)
    compute(0)
    neighbours(3)
    diagonal(2)
    compute(1)
    give_diagonal(0)
    compute(2)
    give_diagonal(1)
    diagonal(3)
    compute(3)
    give_diagonal(2)
    give_diagonal(3)
    give_neighbours(2)
    give_neighbours(3)
    give_neighbours(1)
    give_column(3)
    give_neighbours(0)
    give_column(2)
    give_column(1)
    give_column(0)

    for copy, when in sent:
        if when is None:
            copy.wait_send()
        else:
            pl.when(when)(copy.wait_send)


def fused(
    tokens_in, norm_gain, gate_proj, up_proj, down_proj, route_ids, group_weight, expert_weight
):
    token_count, model_width = tokens_in.shape
    expert_total = gate_proj.shape[0] * lax.axis_size("ep")
    hidden_width = gate_proj.shape[2]
    part = model_width // 2
    half_rows = token_count // 2
    bf16, f32 = jnp.bfloat16, jnp.float32
    dma = pltpu.SemaphoreType.DMA
    vmem, hbm = pl.BlockSpec(memory_space=pltpu.VMEM), pl.BlockSpec(memory_space=pl.ANY)
    blocks = pltpu.VMEM((DEPTH, token_count, part), bf16)
    halves = pltpu.VMEM((DEPTH, half_rows, part), bf16)
    return pl.pallas_call(
        functools.partial(kernel, expert_total),
        out_shape=jax.ShapeDtypeStruct((token_count, part), bf16),
        in_specs=[vmem, vmem, hbm, hbm, hbm, vmem, vmem, vmem],
        out_specs=vmem,
        scratch_shapes=[
            pltpu.VMEM((DEPTH, PLANE, 2, 2, half_rows // 2, model_width + 128), bf16),
            pltpu.VMEM((model_width, hidden_width), bf16),
            pltpu.VMEM((model_width, hidden_width), bf16),
            pltpu.VMEM((hidden_width, model_width), bf16),
            pltpu.VMEM((DEPTH, PLANE, token_count, part), f32),
            pltpu.VMEM((DEPTH, PLANE, token_count, part), bf16),
            pltpu.VMEM((DEPTH, PLANE, token_count, part), bf16),
            pltpu.VMEM((DEPTH, 2, half_rows, part), bf16),
            halves, halves, blocks, blocks, blocks, blocks,
            pltpu.VMEM((token_count, part), f32),
            blocks, blocks, blocks,
            dma((3,)),
            dma((DEPTH, 2)), dma((DEPTH, 2)), dma((DEPTH, 2)),
            dma((DEPTH, 2)), dma((DEPTH, 2)), dma((DEPTH, 2)), dma((DEPTH, 2)),
            dma((DEPTH,)), dma((DEPTH,)), dma((DEPTH,)), dma((DEPTH,)),
            dma((DEPTH, PLANE)), dma((DEPTH, PLANE)),
        ]
        + [dma((DEPTH,))] * 13,
        compiler_params=pltpu.CompilerParams(
            collective_id=0, has_side_effects=True, vmem_limit_bytes=60 * 1024 * 1024
        ),
    )(
        tokens_in, norm_gain.reshape(1, model_width), gate_proj, up_proj, down_proj,
        route_ids, group_weight, expert_weight,
    )


def solution(mesh):
    in_specs = (
        P(("grp", "ep"), None),
        P(),
        P("ep", None, "tp"),
        P("ep", None, "tp"),
        P("ep", "tp", None),
        P(("grp", "ep"), None),
        P(("grp", "ep"), None),
        P(("grp", "ep"), None),
    )
    out_specs = P(("grp", "ep"), "tp")
    relayed = mesh.shape["ep"] == PLANE * DEPTH and mesh.shape["tp"] == 2
    return jax.shard_map(
        fused if relayed else on_device, mesh=mesh, in_specs=in_specs, out_specs=out_specs, check_vma=False
    )
```

```python
import functools

import jax
import jax.numpy as jnp
from jax import lax
from jax.experimental import pallas as pl
from jax.experimental.pallas import tpu as pltpu
from jax.sharding import PartitionSpec as P

TOP = 8
EXP_GRP = 8


EPSILON = 1e-06

MESH = pl.DeviceIdType.MESH
PLANE = 4
DEPTH = 4


def on_device(
    tokens_in, norm_gain, gate_proj, up_proj, down_proj, route_ids, group_weight, expert_weight
):
    token_count, model_width = tokens_in.shape
    expert_count = gate_proj.shape[0] * lax.axis_size("ep")
    lane_count = lax.axis_size("tp")
    part_width = model_width // lane_count
    capacity = min(token_count, max(2, 2 * token_count * TOP // expert_count))
    slot_total = expert_count * capacity
    row_values = tokens_in.astype(jnp.float32)
    inv_scale = lax.rsqrt(jnp.mean(row_values * row_values, axis=-1, keepdims=True) + EPSILON)
    normed = (row_values * inv_scale * norm_gain).astype(jnp.bfloat16)
    route_count = token_count * TOP
    flat_ids = route_ids.reshape(route_count)
    positions = jnp.arange(route_count, dtype=jnp.int32)
    same_expert = (flat_ids[:, None] == flat_ids[None, :]) & (
        positions[None, :] < positions[:, None]
    )
    slot_rank = jnp.sum(same_expert.astype(jnp.int32), axis=1)
    slot_index = flat_ids * capacity + slot_rank
    slot_match = jnp.arange(slot_total, dtype=jnp.int32)[:, None] == slot_index[None, :]
    selector = jnp.sum(
        slot_match.reshape(slot_total, token_count, TOP).astype(jnp.int32), axis=2
    ).astype(jnp.bfloat16)
    gate_local = gate_proj[0]
    up_local = up_proj[0]
    lane_index = lax.axis_index("tp")
    own_half = lax.dynamic_slice_in_dim(normed, lane_index * part_width, part_width, 1)
    outgoing = jnp.dot(selector, own_half, preferred_element_type=jnp.float32).astype(jnp.bfloat16)
    arrived = lax.all_to_all(
        outgoing.reshape(expert_count, capacity, part_width),
        "ep",
        split_axis=0,
        concat_axis=0,
        tiled=True,
    )
    arrived = arrived.reshape(slot_total, part_width)
    column_piece = lax.all_gather(arrived, "tp", axis=1, tiled=True)
    gate_acts = jnp.dot(column_piece, gate_local, preferred_element_type=jnp.float32)
    up_acts = jnp.dot(column_piece, up_local, preferred_element_type=jnp.float32)
    hidden = (jax.nn.silu(gate_acts) * up_acts).astype(jnp.bfloat16)
    partial_rows = jnp.dot(hidden, down_proj[0], preferred_element_type=jnp.float32)
    summed = lax.psum_scatter(
        partial_rows.reshape(expert_count, capacity, model_width).astype(jnp.bfloat16),
        "tp",
        scatter_dimension=2,
        tiled=True,
    )
    returned = lax.all_to_all(summed, "ep", split_axis=0, concat_axis=0, tiled=True).reshape(
        slot_total, part_width
    )
    picked = returned[slot_index].astype(jnp.float32).reshape(token_count, TOP, part_width)
    group_ids = route_ids // EXP_GRP
    group_count = group_weight.shape[1]
    group_match = (
        group_ids[:, :, None] == jnp.arange(group_count, dtype=jnp.int32)[None, None, :]
    ).astype(jnp.float32)
    group_part = jnp.sum(group_weight[:, None, :] * group_match, axis=2)
    gate_values = group_part * expert_weight / jnp.sum(expert_weight, axis=1, keepdims=True)
    return jnp.sum(picked * gate_values[:, :, None], axis=1).astype(jnp.bfloat16)


def plane_order(step, z):
    if step == 0:
        return z
    if step == 1:
        return z + 1 - 2 * (z % 2)
    far = DEPTH - 1 - (DEPTH - 1) * (z // 2)
    return far + (1 - 2 * (1 - z // 2)) * (DEPTH - 1 - step)


def kernel(
    expert_total, tokens_ref, gain_ref, gate_hbm, up_hbm, down_hbm, ids_ref, group_ref, weight_ref,
    out_ref,
    rows, gate_w, up_w, down_w, own_part, give, got, diag_out, diag_x, diag_y, x_out, y_out,
    x_in, y_in, z_total, z_out, z_below, z_above,
    w_sem, up_s, dn_s, z_r, gx_s, gx_r, gy_s, gy_r, dx_s, dx_r, dy_s, dy_r, sib_s, sib_r,
    tp_s, tp_r, rdx_s, rdx_r, rdy_s, rdy_r, rx_s, rx_r, ry_s, ry_r, rz_s, rzb_r, rza_r,
):
    me = lax.axis_index("ep")
    core = lax.axis_index("tp")
    z, q = me // PLANE, me % PLANE
    y, x = q // 2, q % 2
    qx, qy, qd = y * 2 + 1 - x, (1 - y) * 2 + x, (1 - y) * 2 + 1 - x
    x_peer, y_peer = {"ep": z * PLANE + qx}, {"ep": z * PLANE + qy}
    up_peer, dn_peer = {"ep": me + PLANE}, {"ep": me - PLANE}
    sibling = {"tp": 1 - core}
    has_up, has_dn = z < DEPTH - 1, z > 0
    half_rows, width = tokens_ref.shape[0] // 2, tokens_ref.shape[1]
    sub = half_rows // 2
    block = 2 * half_rows
    part = width // 2
    always = None
    sent = []

    weight_copies = [
        pltpu.make_async_copy(src.at[0], dst, w_sem.at[i])
        for i, (src, dst) in enumerate(((gate_hbm, gate_w), (up_hbm, up_w), (down_hbm, down_w)))
    ]
    for copy in weight_copies:
        copy.start()

    barrier = pltpu.get_barrier_semaphore()
    for peer in (x_peer, y_peer, sibling):
        pl.semaphore_signal(barrier, inc=1, device_id=peer, device_id_type=MESH)

    @pl.when(has_up)
    def _():
        pl.semaphore_signal(barrier, inc=1, device_id=up_peer, device_id_type=MESH)

    @pl.when(has_dn)
    def _():
        pl.semaphore_signal(barrier, inc=1, device_id=dn_peer, device_id_type=MESH)

    def send(src, dst, send_sem, recv_sem, peer, when=always):
        copy = pltpu.make_async_remote_copy(
            src_ref=src, dst_ref=dst, send_sem=send_sem, recv_sem=recv_sem,
            device_id=peer, device_id_type=MESH,
        )
        sent.append((copy, when))
        if when is None:
            copy.start()
        else:
            pl.when(when)(copy.start)

    def arrive(dst, recv_sem):
        pltpu.make_async_remote_copy(
            src_ref=dst, dst_ref=dst, send_sem=recv_sem, recv_sem=recv_sem,
            device_id=sibling, device_id_type=MESH,
        ).wait_recv()

    begin = pl.multiple_of(core * half_rows, half_rows)
    values = tokens_ref[pl.ds(begin, half_rows), :].astype(jnp.float32)
    scale = lax.rsqrt(jnp.mean(values * values, axis=-1, keepdims=True) + EPSILON)
    normed = (values * scale * gain_ref[...]).astype(jnp.bfloat16)
    lane = lax.broadcasted_iota(jnp.int32, (half_rows, 128), 1)
    expert = lane % expert_total
    picks = [
        jnp.where(core == 0, turned[0:half_rows], turned[half_rows:])
        for turned in (ids_ref[...].T, weight_ref[...].T, group_ref[...].T)
    ]
    ids, weights, groups = picks
    weights = weights / jnp.sum(weights, axis=1, keepdims=True)
    gates = jnp.zeros((half_rows, 128), jnp.float32)
    for k in range(TOP):
        gates = gates + jnp.where(ids[:, k : k + 1] == expert, weights[:, k : k + 1], 0.0)
    group_part = jnp.zeros((half_rows, 128), jnp.float32)
    for g in range(groups.shape[1]):
        group_part = jnp.where(expert // EXP_GRP == g, groups[:, g : g + 1], group_part)
    gates = gates * group_part
    high = gates.astype(jnp.bfloat16).astype(jnp.float32)
    middle = (gates - high).astype(jnp.bfloat16).astype(jnp.float32)
    low = gates - high - middle
    third = lane // expert_total
    tail = jnp.where(
        third == 0, high, jnp.where(third == 1, middle, jnp.where(third == 2, low, 0.0))
    ).astype(jnp.bfloat16)
    for p in range(2):
        rows[z, q, core, p, :, 0:width] = normed[p * sub : (p + 1) * sub]
        rows[z, q, core, p, :, width:] = tail[p * sub : (p + 1) * sub]

    pl.semaphore_wait(barrier, 3 + jnp.minimum(z, 1) + jnp.minimum(DEPTH - 1 - z, 1))

    def own_column(step):
        at = plane_order(step, z)
        for p in range(2):
            piece = rows.at[at, q, core, p]
            if step > 0:
                arrive(piece, z_r.at[at, p])
            send(piece, piece, up_s.at[at, p], z_r.at[at, p], up_peer, has_up & (at <= z))
            send(piece, piece, dn_s.at[at, p], z_r.at[at, p], dn_peer, has_dn & (at >= z))
            send(piece, piece, gx_s.at[at, p], gx_r.at[at, p], x_peer)
            send(piece, piece, gy_s.at[at, p], gy_r.at[at, p], y_peer)
        to_sibling(at, q)

    def to_sibling(at, column):
        piece = rows.at[at, column, core]
        send(piece, piece, sib_s.at[at, column], sib_r.at[at, column], sibling)

    def neighbours(step):
        at = plane_order(step, z)
        arrive(rows.at[at, qx, core, 0], gx_r.at[at, 0])
        piece = rows.at[at, qx, core, 0]
        send(piece, piece, dy_s.at[at], dy_r.at[at], y_peer)
        arrive(rows.at[at, qy, core, 1], gy_r.at[at, 1])
        piece = rows.at[at, qy, core, 1]
        send(piece, piece, dx_s.at[at], dx_r.at[at], x_peer)
        arrive(rows.at[at, qx, core, 1], gx_r.at[at, 1])
        to_sibling(at, qx)
        arrive(rows.at[at, qy, core, 0], gy_r.at[at, 0])
        to_sibling(at, qy)

    def diagonal(step):
        at = plane_order(step, z)
        arrive(rows.at[at, qd, core, 0], dy_r.at[at])
        arrive(rows.at[at, qd, core, 1], dx_r.at[at])
        to_sibling(at, qd)

    mine = pl.multiple_of(core * part, part)
    other = pl.multiple_of((1 - core) * part, part)

    def compute(step):
        at = plane_order(step, z)
        for column in range(PLANE):
            arrive(rows.at[at, column, 1 - core], sib_r.at[at, column])
        if step == 0:
            for copy in weight_copies:
                copy.wait()
        count = PLANE * block
        taken = rows[at, :, :, :, :, 0:width].reshape(count, width)
        gate_acts = jnp.dot(taken, gate_w[...], preferred_element_type=jnp.float32)
        up_acts = jnp.dot(taken, up_w[...], preferred_element_type=jnp.float32)
        hidden = (gate_acts / (1.0 + jnp.exp(-gate_acts)) * up_acts).astype(jnp.bfloat16)
        tails = rows[at, :, :, :, :, width:].reshape(count, 128).astype(jnp.float32)
        lanes = lax.broadcasted_iota(jnp.int32, (count, 128), 1)
        wanted = (lanes % expert_total == me) & (lanes < 3 * expert_total)
        gate = jnp.sum(jnp.where(wanted, tails, 0.0), axis=1, keepdims=True)
        theirs = jnp.dot(hidden, down_w[:, pl.ds(other, part)], preferred_element_type=jnp.float32)
        give[at] = (theirs * gate).astype(jnp.bfloat16).reshape(PLANE, block, part)
        send(give.at[at], got.at[at], tp_s.at[at], tp_r.at[at], sibling)
        ours = jnp.dot(hidden, down_w[:, pl.ds(mine, part)], preferred_element_type=jnp.float32)
        own_part[at] = (ours * gate).reshape(PLANE, block, part)

    def pair_sum(at, column, half):
        held = pl.ds(half * half_rows, half_rows)
        return own_part[at, column, held] + got[at, column, held].astype(jnp.float32)

    def give_diagonal(step):
        at = plane_order(step, z)
        arrive(got.at[at], tp_r.at[at])
        for half, (dst, send_sem, recv_sem, peer) in enumerate(
            ((diag_x, rdx_s, rdx_r, x_peer), (diag_y, rdy_s, rdy_r, y_peer))
        ):
            diag_out[at, half] = pair_sum(at, qd, half).astype(jnp.bfloat16)
            send(diag_out.at[at, half], dst.at[at], send_sem.at[at], recv_sem.at[at], peer)
        y_out[at, 1] = pair_sum(at, qy, 1).astype(jnp.bfloat16)
        send(y_out.at[at, 1], y_in.at[at, 1], ry_s.at[at, 1], ry_r.at[at, 1], y_peer)
        x_out[at, 0] = pair_sum(at, qx, 0).astype(jnp.bfloat16)
        send(x_out.at[at, 0], x_in.at[at, 0], rx_s.at[at, 0], rx_r.at[at, 0], x_peer)

    def give_neighbours(step):
        at = plane_order(step, z)
        arrive(diag_x.at[at], rdx_r.at[at])
        y_out[at, 0] = (pair_sum(at, qy, 0) + diag_x[at].astype(jnp.float32)).astype(jnp.bfloat16)
        send(y_out.at[at, 0], y_in.at[at, 0], ry_s.at[at, 0], ry_r.at[at, 0], y_peer)
        arrive(diag_y.at[at], rdy_r.at[at])
        x_out[at, 1] = (pair_sum(at, qx, 1) + diag_y[at].astype(jnp.float32)).astype(jnp.bfloat16)
        send(x_out.at[at, 1], x_in.at[at, 1], rx_s.at[at, 1], rx_r.at[at, 1], x_peer)

    def give_column(step):
        at = plane_order(step, z)
        for half in range(2):
            arrive(x_in.at[at, half], rx_r.at[at, half])
            arrive(y_in.at[at, half], ry_r.at[at, half])
            add_planes(step, at, half)

    def add_planes(step, at, half):
        z_total[...] = (
            pair_sum(at, q, half)
            + x_in[at, half].astype(jnp.float32)
            + y_in[at, half].astype(jnp.float32)
        )

        @pl.when(has_dn & (at >= z))
        def _():
            arrive(z_below.at[at, half], rzb_r.at[at, half])
            z_total[...] += z_below[at, half].astype(jnp.float32)

        @pl.when(has_up & (at <= z))
        def _():
            arrive(z_above.at[at, half], rza_r.at[at, half])
            z_total[...] += z_above[at, half].astype(jnp.float32)

        piece = z_out.at[at, half]
        if step == 0:
            out_ref[half * half_rows : (half + 1) * half_rows] = z_total[...].astype(jnp.bfloat16)
        else:
            z_out[at, half] = z_total[...].astype(jnp.bfloat16)
            below, above = z_below.at[at, half], z_above.at[at, half]
            send(piece, below, rz_s.at[at, half], rzb_r.at[at, half], up_peer, at > z)
            send(piece, above, rz_s.at[at, half], rza_r.at[at, half], dn_peer, at < z)

    own_column(0)
    own_column(1)
    own_column(2)
    neighbours(0)
    own_column(3)
    neighbours(1)
    diagonal(0)
    neighbours(2)
    diagonal(1)
    compute(0)
    neighbours(3)
    diagonal(2)
    compute(1)
    give_diagonal(0)
    compute(2)
    give_diagonal(1)
    diagonal(3)
    compute(3)
    give_diagonal(3)
    give_diagonal(2)
    give_neighbours(3)
    give_neighbours(2)
    give_column(3)
    give_neighbours(1)
    give_column(2)
    give_neighbours(0)
    give_column(1)
    give_column(0)

    for copy, when in sent:
        if when is None:
            copy.wait_send()
        else:
            pl.when(when)(copy.wait_send)


def fused(
    tokens_in, norm_gain, gate_proj, up_proj, down_proj, route_ids, group_weight, expert_weight
):
    token_count, model_width = tokens_in.shape
    expert_total = gate_proj.shape[0] * lax.axis_size("ep")
    hidden_width = gate_proj.shape[2]
    part = model_width // 2
    half_rows = token_count // 2
    bf16, f32 = jnp.bfloat16, jnp.float32
    dma = pltpu.SemaphoreType.DMA
    vmem, hbm = pl.BlockSpec(memory_space=pltpu.VMEM), pl.BlockSpec(memory_space=pl.ANY)
    blocks = pltpu.VMEM((DEPTH, 2, half_rows, part), bf16)
    halves = pltpu.VMEM((DEPTH, half_rows, part), bf16)
    return pl.pallas_call(
        functools.partial(kernel, expert_total),
        out_shape=jax.ShapeDtypeStruct((token_count, part), bf16),
        in_specs=[vmem, vmem, hbm, hbm, hbm, vmem, vmem, vmem],
        out_specs=vmem,
        scratch_shapes=[
            pltpu.VMEM((DEPTH, PLANE, 2, 2, half_rows // 2, model_width + 128), bf16),
            pltpu.VMEM((model_width, hidden_width), bf16),
            pltpu.VMEM((model_width, hidden_width), bf16),
            pltpu.VMEM((hidden_width, model_width), bf16),
            pltpu.VMEM((DEPTH, PLANE, token_count, part), f32),
            pltpu.VMEM((DEPTH, PLANE, token_count, part), bf16),
            pltpu.VMEM((DEPTH, PLANE, token_count, part), bf16),
            pltpu.VMEM((DEPTH, 2, half_rows, part), bf16),
            halves, halves, blocks, blocks, blocks, blocks,
            pltpu.VMEM((half_rows, part), f32),
            blocks, blocks, blocks,
            dma((3,)),
            dma((DEPTH, 2)), dma((DEPTH, 2)), dma((DEPTH, 2)),
            dma((DEPTH, 2)), dma((DEPTH, 2)), dma((DEPTH, 2)), dma((DEPTH, 2)),
            dma((DEPTH,)), dma((DEPTH,)), dma((DEPTH,)), dma((DEPTH,)),
            dma((DEPTH, PLANE)), dma((DEPTH, PLANE)),
        ]
        + [dma((DEPTH,))] * 6
        + [dma((DEPTH, 2))] * 7,
        compiler_params=pltpu.CompilerParams(
            collective_id=0, has_side_effects=True, vmem_limit_bytes=60 * 1024 * 1024
        ),
    )(
        tokens_in, norm_gain.reshape(1, model_width), gate_proj, up_proj, down_proj,
        route_ids.T, group_weight.T, expert_weight.T,
    )


def solution(mesh):
    in_specs = (
        P(("grp", "ep"), None),
        P(),
        P("ep", None, "tp"),
        P("ep", None, "tp"),
        P("ep", "tp", None),
        P(("grp", "ep"), None),
        P(("grp", "ep"), None),
        P(("grp", "ep"), None),
    )
    out_specs = P(("grp", "ep"), "tp")
    relayed = mesh.shape["ep"] == PLANE * DEPTH and mesh.shape["tp"] == 2
    return jax.shard_map(
        fused if relayed else on_device, mesh=mesh, in_specs=in_specs, out_specs=out_specs, check_vma=False
    )
```
